32 devices in a mesh: ep: 8 (over z, y), tp: 4 (over x, core).
Axes of the slice: x: 2, y: 2, z: 4, core: 2. Of those that a mesh axis runs over, the one named last changes fastest.
Arguments:
- queries: bfloat16 [16384, 1024], P('ep', 'tp'), may hold values from -6 to 6
- keys_values: bfloat16 [16384, 512], P('ep', 'tp'), may hold values from -6 to 6
- sink_logits: float32 [16], replicated, may hold values from 4 to 8
- out_weight: bfloat16 [1024, 2048], replicated, may hold values from -4 to 4
- expert_tokens: bfloat16 [8192, 2048], P(('ep', 'tp')), may hold values from -6 to 6
- norm_gain: float32 [2048], replicated, may hold values from 0.1 to 1.9
- routes: int32 [8192, 2], P(('ep', 'tp')), may hold values from 0 to 7, all different within a row; in each aligned block of 256 rows (0 to 255, 256 to 511, ...) at most 96 rows name the same one
- route_weights: float32 [8192, 2], P(('ep', 'tp')), may hold values from 0.1 to 1
- gate_weight: bfloat16 [8, 2048, 1024], P('ep', None, 'tp'), may hold values from -0.125 to 0.125
- up_weight: bfloat16 [8, 2048, 1024], P('ep', None, 'tp'), may hold values from -0.125 to 0.125
- down_weight: bfloat16 [8, 1024, 2048], P('ep', 'tp'), may hold values from -0.1875 to 0.1875
Outputs:
- mixer_out: bfloat16 [16384, 2048], P(('ep', 'tp'))
- expert_out: bfloat16 [8192, 2048], P(('ep', 'tp'))
The draws below stay inside these ranges and needn't reach their ends.
Inputs may be any that keep to these rules, and one draw needn't show every extreme that they name: `routes`: each row names 2 different experts. In each aligned block of 256 rows, no expert is named by more than 96 rows, and in some block an expert is named by exactly 96 rows.
All inputs are finite; a program needn't handle non-finite values.
Results may differ from the reference program's by a relative error of at most 0.012.
Values may be sent and summed in bfloat16 or wider, within the bound.
No kernel may reach another device: no remote copies, remote signals or barrier semaphores. Data moves between devices by JAX's collectives and lax.ppermute only.
A program may use at most 128 MiB of HBM per device.

```python
import math
import jax
import jax.numpy as jnp
import numpy as np
from jax import lax

D = 2048
HEADS = 16
KV_HEADS = 4
GROUP = 4
HEAD_DIM = 64
WINDOW = 128
FE = 1024
TOPK = 2
MOE_ROWS = 256
SEQ = 16384
MOE_TOKENS = 8192
EXPERTS = 8
CAP = 96
N_TP = 4


def draw_queries(key, part):
    noise_key = jax.random.fold_in(key, 11)
    return jax.random.truncated_normal(noise_key, -6.0, 6.0, (SEQ, HEADS * HEAD_DIM)).astype(jnp.bfloat16)


def draw_keys_values(key, part):
    noise_key = jax.random.fold_in(key, 17)
    return jax.random.truncated_normal(noise_key, -6.0, 6.0, (SEQ, KV_HEADS * 2 * HEAD_DIM)).astype(jnp.bfloat16)


def block_scale(key, shape, split, least, high):
    level = 1.0
    for axis_at, shards_of in split:
        draws = jax.random.uniform(jax.random.fold_in(jax.random.fold_in(key, 6), axis_at), (shards_of,), jnp.float32, least / len(split), high / len(split))
        level = level * jnp.repeat(jnp.exp(draws), shape[axis_at] // shards_of).reshape((-1,) + (1,) * (len(shape) - 1 - axis_at))
    return level


def routed_block(own_key, own, number, rows, number_of, top, most, lean):
    order = jax.random.permutation(own_key, number_of)
    crowded, usual = portions_of(number_of, rows * top, most, lean, True), portions_of(number_of, rows * top, most, lean, False)
    places = jnp.arange(number_of)

    def named(lengths, rotation):
        used = int((lengths > 0).sum())
        fixed = max(1, used // 4)
        moved = fixed + (places - fixed + rotation * (used - fixed)) % max(1, number_of - fixed)
        return jnp.zeros((number_of,), jnp.int32).at[order[jnp.where(places < fixed, places, moved)]].set(jnp.asarray(lengths, jnp.int32))

    lengths = jnp.where(number % 4 == 0, named(crowded, number // 4), named(usual, number - number // 4 - 1))
    mixed = jax.random.permutation(jax.random.fold_in(own, 3), number_of)
    giver, taker = mixed[0:number_of // 2 * 2:2], mixed[1:number_of // 2 * 2:2]
    margin = jnp.minimum(lengths[giver] - 1, most - lengths[taker]) // 2
    margin = jnp.where((giver == order[0]) | (taker == order[0]) | (lengths[taker] == 0), 0, jnp.maximum(margin, 0))
    moved = jax.random.randint(jax.random.fold_in(own, 4), (number_of // 2,), 0, 1 << 20) % (margin + 1)
    lengths = lengths.at[giver].add(-moved).at[taker].add(moved)
    items = jnp.searchsorted(jnp.cumsum(lengths), jnp.arange(rows * top), side="right").astype(jnp.int32)
    table = items.reshape(top, rows).T
    table = table[jax.random.permutation(jax.random.fold_in(own, 1), rows)]
    rotation = jax.random.randint(jax.random.fold_in(own, 2), (rows, 1), 0, top)
    return jnp.take_along_axis(table, (jnp.arange(top)[None, :] + rotation) % top, axis=1)


def portions_of(number_of, total, most, skew, full):
    portions = [(1 << 20) // math.isqrt(grade ** skew) + 1 for grade in range(1, number_of + 1)]
    largest = most if full else min(most, max(-(-total // number_of), total * portions[0] // sum(portions)))
    least = 1 if total - largest >= number_of - 1 else 0
    counts, surplus = [largest] + [least] * (number_of - 1), total - largest - least * (number_of - 1)
    while surplus > 0:
        candidates = [i for i in range(1, number_of) if counts[i] < largest] or [i for i in range(1, number_of) if counts[i] < most]
        whole, left = sum([portions[i] for i in candidates]), surplus
        for i in candidates:
            addition = min(most - counts[i], max(1, left * portions[i] // whole), surplus)
            counts[i] = counts[i] + addition
            surplus = surplus - addition
    return np.array(counts)


def normal_values(rng, dims, width, limit, cuts=(), kind=jnp.bfloat16):
    result = width * jax.random.normal(rng, dims, jnp.float32)
    if cuts:
        result = result * block_scale(rng, dims, cuts, -0.22, 0.18)
    return jnp.clip(result, -limit, limit).astype(kind)


def setup_inputs(seed: int = 0) -> dict:
    keys = jax.random.split(jax.random.key(seed), 12)
    queries = draw_queries(jax.random.fold_in(keys[11], 71), 0)
    keys_values = draw_keys_values(jax.random.fold_in(keys[11], 71), 0)
    sink_logits = jnp.clip(jax.random.uniform(keys[2], (HEADS,), jnp.float32, 4.0, 8.0), 4.0, 8.0)
    out_weight = normal_values(keys[3], (HEADS * HEAD_DIM, D), 0.8, 4.0)
    expert_tokens = normal_values(keys[4], (MOE_TOKENS, D), 1.0, 6.0, ((0, 32),))
    norm_gain = jnp.clip(1.0 + 0.18 * jax.random.normal(keys[5], (D,), jnp.float32), 0.1, 1.9)
    routes_keys = jax.random.split(jax.random.fold_in(keys[6], 1), MOE_TOKENS // MOE_ROWS)
    routes_turns = jax.random.permutation(jax.random.fold_in(keys[6], 3), MOE_TOKENS // MOE_ROWS)
    routes = jax.vmap(lambda own, number: routed_block(jax.random.fold_in(keys[6], 2), own, number, MOE_ROWS, EXPERTS, TOPK, CAP, 2))(routes_keys, routes_turns).reshape((MOE_TOKENS, TOPK))
    route_weights = jnp.clip(0.1 + 0.9 * jax.random.uniform(keys[7], (MOE_TOKENS, TOPK), jnp.float32) ** block_scale(keys[7], (MOE_TOKENS, TOPK), ((0, 32),), -0.2, 0.2), 0.1, 1.0)
    gate_weight = normal_values(keys[8], (EXPERTS, D, FE), D ** -0.5, 0.125, ((0, 8), (2, 4)))
    up_weight = normal_values(keys[9], (EXPERTS, D, FE), D ** -0.5, 0.125, ((0, 8), (2, 4)))
    down_weight = normal_values(keys[10], (EXPERTS, FE, D), FE ** -0.5, 0.1875, ((0, 8), (1, 4)))
    return dict(queries=queries, keys_values=keys_values, sink_logits=sink_logits, out_weight=out_weight, expert_tokens=expert_tokens, norm_gain=norm_gain, routes=routes, route_weights=route_weights, gate_weight=gate_weight, up_weight=up_weight, down_weight=down_weight)


NEG_FILL = -1e+30

def attend_all(queries, keys_values, sink_logits):
    seq_total = queries.shape[0]
    block_rows = min(512, seq_total)
    key_span = block_rows + 2 * WINDOW
    query_all = queries.astype(jnp.float32).reshape(seq_total, KV_HEADS, GROUP, HEAD_DIM)
    pair_all = keys_values.astype(jnp.float32).reshape(seq_total, KV_HEADS, 2, HEAD_DIM)
    padded = jnp.pad(pair_all, ((WINDOW, WINDOW), (0, 0), (0, 0), (0, 0)))
    sink_grid = sink_logits.astype(jnp.float32).reshape(KV_HEADS, GROUP, 1, 1)

    def one_block(block_index):
        first_row = block_index * block_rows
        query_block = lax.dynamic_slice_in_dim(query_all, first_row, block_rows, 0)
        pair_block = lax.dynamic_slice_in_dim(padded, first_row, key_span, 0)
        scores = jnp.einsum('qhgd,khd->hgqk', query_block, pair_block[:, :, 0]) * HEAD_DIM ** (-0.5)
        query_pos = first_row + jnp.arange(block_rows, dtype=jnp.int32)
        key_pos = first_row - WINDOW + jnp.arange(key_span, dtype=jnp.int32)
        allowed = (jnp.abs(query_pos[:, None] - key_pos[None, :]) <= WINDOW) & (key_pos >= 0)[None, :] & (key_pos < seq_total)[None, :]
        scores = jnp.where(allowed, scores, NEG_FILL)
        top_score = jnp.maximum(lax.optimization_barrier(jnp.max(scores, -1, keepdims=True)), sink_grid)
        exp_scores = jnp.exp(scores - top_score)
        denominator = lax.optimization_barrier(jnp.sum(exp_scores, -1, keepdims=True)) + jnp.exp(sink_grid - top_score)
        attn_weights = lax.optimization_barrier((exp_scores / denominator).astype(jnp.bfloat16)).astype(jnp.float32)
        head_values = jnp.einsum('hgqk,khd->qhgd', attn_weights, pair_block[:, :, 1])
        return head_values.astype(jnp.bfloat16).reshape(block_rows, HEADS * HEAD_DIM)
    blocks = lax.map(one_block, jnp.arange(seq_total // block_rows, dtype=jnp.int32))
    return blocks.reshape(seq_total, HEADS * HEAD_DIM)

def reference(queries, keys_values, sink_logits, out_weight, expert_tokens, norm_gain, routes, route_weights, gate_weight, up_weight, down_weight):
    attended = attend_all(queries, keys_values, sink_logits)
    mixer_out = jnp.dot(attended, out_weight, preferred_element_type=jnp.float32).astype(jnp.bfloat16)
    token_total = expert_tokens.shape[0]
    block_count = token_total // MOE_ROWS
    rows_float = expert_tokens.astype(jnp.float32)
    centred = rows_float - lax.optimization_barrier(jnp.mean(rows_float, -1, keepdims=True))
    normed = (centred * lax.rsqrt(lax.optimization_barrier(jnp.mean(centred * centred, -1, keepdims=True)) + 1e-06) * norm_gain).astype(jnp.bfloat16)
    flat_routes = routes.reshape(block_count, MOE_ROWS * TOPK).astype(jnp.int32)
    one_hot = (flat_routes[:, :, None] == jnp.arange(EXPERTS, dtype=jnp.int32)[None, None, :]).astype(jnp.int32)
    slot_rank = lax.optimization_barrier(jnp.sum((jnp.cumsum(one_hot, 1) - 1) * one_hot, -1))
    block_ids = jnp.arange(block_count, dtype=jnp.int32)[:, None]
    expert_slot = (flat_routes * (block_count * CAP) + block_ids * CAP + slot_rank).reshape(-1)
    copy_token = (block_ids * MOE_ROWS + jnp.arange(MOE_ROWS * TOPK, dtype=jnp.int32)[None, :] // TOPK).reshape(-1)
    slot_table = jnp.full((EXPERTS * block_count * CAP,), token_total, jnp.int32).at[expert_slot].set(copy_token)
    slot_table = slot_table.reshape(EXPERTS, block_count * CAP)
    weight_table = jnp.zeros((EXPERTS * block_count * CAP,), jnp.float32).at[expert_slot].set(route_weights.reshape(-1))
    weight_table = weight_table.reshape(EXPERTS, block_count * CAP)
    quarter = FE // N_TP

    def add_expert(running, expert_index):
        token_index = slot_table[expert_index]
        chosen = jnp.take(normed, token_index, axis=0, mode='fill', fill_value=0)
        gate_value = jnp.dot(chosen, gate_weight[expert_index], preferred_element_type=jnp.float32)
        up_value = jnp.dot(chosen, up_weight[expert_index], preferred_element_type=jnp.float32)
        hidden = (jax.nn.silu(gate_value) * up_value).astype(jnp.bfloat16)
        hidden_parts = hidden.astype(jnp.float32).reshape(-1, N_TP, quarter)
        down_parts = down_weight[expert_index].astype(jnp.float32).reshape(N_TP, quarter, -1)
        partial_value = jnp.einsum('rqf,qfd->qrd', hidden_parts, down_parts)
        partial_value = lax.optimization_barrier(partial_value.astype(jnp.bfloat16)).astype(jnp.float32)
        copy_result = lax.optimization_barrier(jnp.sum(partial_value, 0)).astype(jnp.bfloat16)
        update = lax.optimization_barrier(copy_result).astype(jnp.float32) * weight_table[expert_index][:, None]
        return (running.at[token_index].add(update, mode='drop'), None)
    total_out, unused = lax.scan(add_expert, jnp.zeros((token_total, expert_tokens.shape[1]), jnp.float32), jnp.arange(EXPERTS, dtype=jnp.int32))
    expert_out = total_out.astype(jnp.bfloat16)
    return (mixer_out, expert_out)
```

```python
import math

import jax
import jax.numpy as jnp
from jax import lax
from jax.experimental import pallas as pl
from jax.experimental.pallas import tpu as pltpu
from jax.sharding import PartitionSpec as P


HEAD_DIM = 64
WINDOW = 128
TOPK = 2
CHUNKS = 2


NEG_FILL = -1e30


def padded_2(cells, sides, width):
    for axis, dim in sides:
        count = lax.axis_size(axis)
        ends = count - 1
        head = lax.slice_in_dim(cells, 0, width, axis=dim)
        tail = lax.slice_in_dim(cells, cells.shape[dim] - width, cells.shape[dim], axis=dim)
        cells = jnp.concatenate(
            [
                lax.ppermute(tail, axis, [(i, (i + 1) % count) for i in range(ends)]),
                cells,
                lax.ppermute(head, axis, [((i + 1) % count, i) for i in range(ends)]),
            ],
            axis=dim,
        )
    return cells


def gathered_parts(blocks, axis):
    count = lax.axis_size(axis)
    groups = {0: blocks}
    bit = count // 2
    while bit:
        pairs = [(i, i ^ bit) for i in range(count)]
        for held in sorted(groups):
            groups[held ^ bit] = tuple(lax.ppermute(block, axis, pairs) for block in groups[held])
        bit = bit // 2
    return [groups[held] for held in sorted(groups)]


def dispatch_kernel(tokens_ref, gain_ref, slots_ref, *out_refs):
    rows_float = tokens_ref[...].astype(jnp.float32)
    centred = rows_float - jnp.mean(rows_float, -1, keepdims=True)
    normed = (
        centred
        * lax.rsqrt(jnp.mean(centred * centred, -1, keepdims=True) + 1e-06)
        * gain_ref[...]
    ).astype(jnp.bfloat16)
    peers = slots_ref.shape[0]
    chunk = out_refs[0].shape[0]
    place = lax.broadcasted_iota(jnp.int32, (chunk, rows_float.shape[0]), 0)
    for number in range(len(out_refs) // peers):
        picks = [
            jnp.where(slots_ref[peer : peer + 1, :] == place + number * chunk, 1.0, 0.0)
            for peer in range(peers)
        ]
        chosen = jnp.dot(
            jnp.concatenate(picks, 0).astype(jnp.bfloat16),
            normed,
            preferred_element_type=jnp.float32,
        ).astype(jnp.bfloat16)
        for peer in range(peers):
            out_refs[number * peers + peer][...] = chosen[peer * chunk : (peer + 1) * chunk]


def dispatch(tokens, gain, slots, chunk, chunks):
    peers, row_count = slots.shape
    width = tokens.shape[1]
    sent = pl.pallas_call(
        dispatch_kernel,
        out_shape=[jax.ShapeDtypeStruct((chunk, width), jnp.bfloat16)] * (peers * chunks),
        cost_estimate=pl.CostEstimate(
            flops=2 * peers * chunks * chunk * row_count * width,
            bytes_accessed=2 * tokens.size + 2 * peers * chunks * chunk * width,
            transcendentals=row_count,
        ),
        name="dispatch",
    )(tokens, gain.reshape(1, width), slots)
    return [sent[number * peers : (number + 1) * peers] for number in range(chunks)]


def exchange(blocks, axis):
    count = lax.axis_size(axis)
    swapped = {
        k: lax.ppermute(blocks[k], axis, [(i, i ^ k) for i in range(count)])
        for k in range(count - 1, 0, -1)
    }
    return [blocks[0]] + [swapped[k] for k in range(1, count)]


def expert_kernel(*refs, peers, count):
    row_refs, sources, out_refs = refs[:peers], refs[peers : peers + count], refs[peers + count :]
    out_refs, held = out_refs[:peers], out_refs[peers:]
    rows_held, total_ref, arrivals = held[count:]
    row_copies = [
        pltpu.make_async_copy(source, rows_held.at[peer], arrivals.at[count + peer])
        for peer, source in enumerate(row_refs)
    ]
    copies = [
        pltpu.make_async_copy(source, place, arrivals.at[number])
        for number, (source, place) in enumerate(zip(sources, held))
    ]
    for copy in row_copies + copies:
        copy.start()
    for copy in row_copies:
        copy.wait()
    chunk, width = row_refs[0].shape
    rows = rows_held[...].reshape(peers * chunk, width)
    for number in range(0, count, 3):
        copies[number].wait()
        gate_value = jnp.dot(rows, held[number][...], preferred_element_type=jnp.float32)
        copies[number + 1].wait()
        up_value = jnp.dot(rows, held[number + 1][...], preferred_element_type=jnp.float32)
        hidden = (gate_value / (1.0 + jnp.exp(-gate_value)) * up_value).astype(jnp.bfloat16)
        copies[number + 2].wait()
        part = jnp.dot(hidden, held[number + 2][...], preferred_element_type=jnp.float32)
        if number + 3 < count:
            total_ref[...] = part if number == 0 else total_ref[...] + part
        else:
            total = (total_ref[...] + part if number else part).astype(jnp.bfloat16)
            for peer in range(peers):
                out_refs[peer][...] = total[peer * chunk : (peer + 1) * chunk]


def expert_chunk(blocks, parts):
    flat = [array for part in parts for array in part]
    peers = len(blocks)
    chunk, width = blocks[0].shape
    row_count = peers * chunk
    hidden_units = sum(part[0].shape[1] for part in parts)
    return pl.pallas_call(
        lambda *refs: expert_kernel(*refs, peers=peers, count=len(flat)),
        out_shape=[jax.ShapeDtypeStruct((chunk, width), jnp.bfloat16)] * peers,
        in_specs=[pl.BlockSpec(memory_space=pl.ANY)] * (peers + len(flat)),
        scratch_shapes=[pltpu.VMEM(array.shape, array.dtype) for array in flat]
        + [
            pltpu.VMEM((peers, chunk, width), jnp.bfloat16),
            pltpu.VMEM((row_count, width), jnp.float32),
            pltpu.SemaphoreType.DMA((len(flat) + peers,)),
        ],
        cost_estimate=pl.CostEstimate(
            flops=6 * row_count * width * hidden_units,
            bytes_accessed=sum(2 * array.size for array in flat) + 4 * row_count * width,
            transcendentals=row_count * hidden_units,
        ),
        name="expert",
    )(*blocks, *flat)


def combine_kernel(shares_ref, *refs, peers):
    block_refs, rest = refs[:peers], refs[peers:]
    out_ref, held, arrivals = rest[-3:]
    copies = [
        pltpu.make_async_copy(source, held.at[peer], arrivals.at[peer])
        for peer, source in enumerate(block_refs)
    ]
    for copy in copies:
        copy.start()
    for copy in copies:
        copy.wait()
    chunk, width = block_refs[0].shape
    both = jnp.dot(
        shares_ref[...],
        held[...].reshape(peers * chunk, width),
        preferred_element_type=jnp.float32,
    )
    row_count = out_ref.shape[0]
    total = both[:row_count] + both[row_count:]
    if len(rest) > 3:
        total = total + rest[0][...]
    out_ref[...] = total.astype(out_ref.dtype)


def combine(shares, blocks, earlier, kind):
    peers = len(blocks)
    chunk, width = blocks[0].shape
    row_count = shares.shape[0] // 2
    whole = pl.BlockSpec(memory_space=pltpu.VMEM)
    return pl.pallas_call(
        lambda *refs: combine_kernel(*refs, peers=peers),
        out_shape=jax.ShapeDtypeStruct((row_count, width), kind),
        in_specs=[whole] + [pl.BlockSpec(memory_space=pl.ANY)] * peers + [whole] * len(earlier),
        scratch_shapes=[
            pltpu.VMEM((peers, chunk, width), jnp.bfloat16),
            pltpu.SemaphoreType.DMA((peers,)),
        ],
        cost_estimate=pl.CostEstimate(
            flops=4 * row_count * peers * chunk * width,
            bytes_accessed=2 * peers * chunk * width + 6 * row_count * width,
            transcendentals=0,
        ),
        name="combine",
    )(shares, *blocks, *earlier)


def attend_kernel(limits_ref, sinks_ref, query_ref, pairs_ref, out_ref, *, group_size):
    block = pl.program_id(0)
    step = WINDOW
    span = step + 2 * WINDOW
    wide = 2 * HEAD_DIM
    scale = HEAD_DIM ** (-0.5) * math.log2(math.e)
    query_at = lax.broadcasted_iota(jnp.int32, (step, span), 0)
    key_at = lax.broadcasted_iota(jnp.int32, (step, span), 1)
    band = (key_at >= query_at) & (key_at <= query_at + 2 * WINDOW)
    low_half = lax.broadcasted_iota(jnp.int32, (span, wide), 1) < HEAD_DIM
    for part in range(query_ref.shape[0] // step):
        first = pl.multiple_of(block * query_ref.shape[0] + part * step, step)
        allowed = (
            band & (key_at >= limits_ref[0] - first) & (key_at < limits_ref[1] - first)
        )
        for kv_head in range(pairs_ref.shape[1] // wide):
            pair = pairs_ref[pl.ds(first, span), kv_head * wide : (kv_head + 1) * wide]
            turned = jnp.concatenate([pair[:, HEAD_DIM:], pair[:, :HEAD_DIM]], axis=1)
            zero = jnp.zeros_like(pair)
            keys = (jnp.where(low_half, pair, zero), jnp.where(low_half, zero, turned))
            values = (jnp.where(low_half, turned, zero), jnp.where(low_half, zero, pair))
            for two in range(group_size // 2):
                column = (kv_head * group_size + 2 * two) * HEAD_DIM
                query = query_ref[part * step : (part + 1) * step, column : column + wide]
                both = None
                for side in range(2):
                    sink = sinks_ref[kv_head * group_size + 2 * two + side]
                    scores = lax.dot_general(
                        query,
                        keys[side],
                        (((1,), (1,)), ((), ())),
                        preferred_element_type=jnp.float32,
                    )
                    scores = jnp.where(allowed, scores * scale, NEG_FILL)
                    top = jnp.maximum(jnp.max(scores, -1, keepdims=True), sink)
                    grown = jnp.exp2(scores - top)
                    denominator = jnp.sum(grown, -1, keepdims=True) + jnp.exp2(sink - top)
                    head = jnp.dot(
                        grown.astype(jnp.bfloat16),
                        values[side],
                        preferred_element_type=jnp.float32,
                    ) * (1.0 / denominator)
                    both = head if both is None else both + head
                out_ref[part * step : (part + 1) * step, column : column + wide] = both.astype(
                    out_ref.dtype
                )


def attend(queries, padded, sink_logits):
    row_count, width = queries.shape
    kv_local = padded.shape[1] // (2 * HEAD_DIM)
    group_size = width // (kv_local * HEAD_DIM)
    block_rows = min(2 * WINDOW, row_count)
    offset = lax.axis_index("ep") * row_count
    seq_total = row_count * lax.axis_size("ep")
    limits = jnp.stack([WINDOW - offset, seq_total + WINDOW - offset]).astype(jnp.int32)
    heads = kv_local * group_size
    sinks = lax.dynamic_slice_in_dim(sink_logits, lax.axis_index("tp") * heads, heads, 0)
    return pl.pallas_call(
        lambda *refs: attend_kernel(*refs, group_size=group_size),
        out_shape=jax.ShapeDtypeStruct(queries.shape, jnp.bfloat16),
        grid=(row_count // block_rows,),
        in_specs=[
            pl.BlockSpec(memory_space=pltpu.SMEM),
            pl.BlockSpec(memory_space=pltpu.SMEM),
            pl.BlockSpec((block_rows, width), lambda i: (i, 0)),
            pl.BlockSpec(padded.shape, lambda i: (0, 0)),
        ],
        out_specs=pl.BlockSpec((block_rows, width), lambda i: (i, 0)),
        cost_estimate=pl.CostEstimate(
            flops=24 * row_count * width * WINDOW,
            bytes_accessed=4 * queries.size + 2 * padded.size,
            transcendentals=3 * row_count * heads * WINDOW,
        ),
        name="attend",
    )(limits, sinks * math.log2(math.e), queries, padded)


def layer(
    queries,
    keys_values,
    sink_logits,
    out_weight,
    expert_tokens,
    norm_gain,
    routes,
    route_weights,
    gate_weight,
    up_weight,
    down_weight,
):
    ep_count = lax.axis_size("ep")
    padded = padded_2(keys_values, (("ep", 0),), WINDOW)
    weights = gathered_parts((gate_weight[0], up_weight[0], down_weight[0]), "tp")

    row_count = expert_tokens.shape[0]
    capacity = 3 * row_count * TOPK // (2 * ep_count)
    chunk = -(-capacity // (CHUNKS * 16)) * 16

    order = lax.axis_index("ep") ^ jnp.arange(ep_count, dtype=jnp.int32)
    named_each = routes[:, :, None] == order
    named = jnp.any(named_each, 1)
    copy_weight = jnp.sum(jnp.where(named_each, route_weights[:, :, None], 0.0), 1)
    places = jnp.arange(row_count, dtype=jnp.int32)
    earlier = (places[None, :] < places[:, None]).astype(jnp.bfloat16)
    rank = jnp.dot(earlier, named.astype(jnp.bfloat16), preferred_element_type=jnp.float32)
    slot = jnp.where(named, rank.astype(jnp.int32), -1)

    sent = dispatch(expert_tokens, norm_gain, slot.T, chunk, CHUNKS)
    arrived = []
    for number in range(CHUNKS):
        arrived.append(exchange(sent[number], "ep"))

    attended = attend(queries, padded, sink_logits)
    tp_count = lax.axis_size("tp")
    mine = lax.axis_index("tp")
    own_rows = attended.shape[0] // tp_count
    width = attended.shape[1]
    mixer_sum = None
    for other in range(tp_count):
        rows = lax.dynamic_slice_in_dim(attended, (mine ^ other) * own_rows, own_rows, 0)
        if other:
            rows = lax.ppermute(rows, "tp", [(i, i ^ other) for i in range(tp_count)])
        part = jnp.dot(
            rows,
            lax.dynamic_slice_in_dim(out_weight, (mine ^ other) * width, width, 0),
            preferred_element_type=jnp.float32,
        )
        mixer_sum = part if mixer_sum is None else mixer_sum + part
    mixer_out = mixer_sum.astype(jnp.bfloat16)

    gathered = ()
    for number in range(CHUNKS):
        results = expert_chunk(arrived[number], weights)
        returned = exchange(results, "ep")
        slots = number * chunk + jnp.arange(chunk, dtype=jnp.int32)
        share = jnp.where(
            slot[:, :, None] == slots[None, None, :], copy_weight[:, :, None], 0.0
        ).reshape(row_count, ep_count * chunk)
        share_high = lax.reduce_precision(share, 8, 7)
        shares = jnp.concatenate([share_high, share - share_high], 0).astype(jnp.bfloat16)
        last = number == CHUNKS - 1
        gathered = (
            combine(shares, returned, gathered, jnp.bfloat16 if last else jnp.float32),
        )
    return (mixer_out, gathered[0])


def solution(mesh):
    return jax.shard_map(
        layer,
        mesh=mesh,
        in_specs=(
            P("ep", "tp"),
            P("ep", "tp"),
            P(),
            P(),
            P(("ep", "tp"), None),
            P(),
            P(("ep", "tp"), None),
            P(("ep", "tp"), None),
            P("ep", None, "tp"),
            P("ep", None, "tp"),
            P("ep", "tp", None),
        ),
        out_specs=(P(("ep", "tp"), None), P(("ep", "tp"), None)),
        check_vma=False,
    )
```

```python
import math

import jax
import jax.numpy as jnp
from jax import lax
from jax.experimental import pallas as pl
from jax.experimental.pallas import tpu as pltpu
from jax.sharding import PartitionSpec as P


HEAD_DIM = 64
WINDOW = 128
TOPK = 2
CHUNKS = 2


NEG_FILL = -1e30


def padded_2(cells, sides, width):
    for axis, dim in sides:
        count = lax.axis_size(axis)
        ends = count - 1
        head = lax.slice_in_dim(cells, 0, width, axis=dim)
        tail = lax.slice_in_dim(cells, cells.shape[dim] - width, cells.shape[dim], axis=dim)
        cells = jnp.concatenate(
            [
                lax.ppermute(tail, axis, [(i, (i + 1) % count) for i in range(ends)]),
                cells,
                lax.ppermute(head, axis, [((i + 1) % count, i) for i in range(ends)]),
            ],
            axis=dim,
        )
    return cells


def gathered_parts(blocks, axis):
    count = lax.axis_size(axis)
    groups = {0: blocks}
    bit = count // 2
    while bit:
        pairs = [(i, i ^ bit) for i in range(count)]
        for held in sorted(groups):
            groups[held ^ bit] = tuple(lax.ppermute(block, axis, pairs) for block in groups[held])
        bit = bit // 2
    return [groups[held] for held in sorted(groups)]


def dispatch_kernel(tokens_ref, gain_ref, slots_ref, *out_refs):
    rows_float = tokens_ref[...].astype(jnp.float32)
    centred = rows_float - jnp.mean(rows_float, -1, keepdims=True)
    normed = (
        centred
        * lax.rsqrt(jnp.mean(centred * centred, -1, keepdims=True) + 1e-06)
        * gain_ref[...]
    ).astype(jnp.bfloat16)
    peers = slots_ref.shape[0]
    chunk = out_refs[0].shape[0]
    place = lax.broadcasted_iota(jnp.int32, (chunk, rows_float.shape[0]), 0)
    for number in range(len(out_refs) // peers):
        picks = [
            jnp.where(slots_ref[peer : peer + 1, :] == place + number * chunk, 1.0, 0.0)
            for peer in range(peers)
        ]
        chosen = jnp.dot(
            jnp.concatenate(picks, 0).astype(jnp.bfloat16),
            normed,
            preferred_element_type=jnp.float32,
        ).astype(jnp.bfloat16)
        for peer in range(peers):
            out_refs[number * peers + peer][...] = chosen[peer * chunk : (peer + 1) * chunk]


def dispatch(tokens, gain, slots, chunk, chunks):
    peers, row_count = slots.shape
    width = tokens.shape[1]
    sent = pl.pallas_call(
        dispatch_kernel,
        out_shape=[jax.ShapeDtypeStruct((chunk, width), jnp.bfloat16)] * (peers * chunks),
        cost_estimate=pl.CostEstimate(
            flops=2 * peers * chunks * chunk * row_count * width,
            bytes_accessed=2 * tokens.size + 2 * peers * chunks * chunk * width,
            transcendentals=row_count,
        ),
        name="dispatch",
    )(tokens, gain.reshape(1, width), slots)
    return [sent[number * peers : (number + 1) * peers] for number in range(chunks)]


def exchange(blocks, axis):
    count = lax.axis_size(axis)
    swapped = {
        k: lax.ppermute(blocks[k], axis, [(i, i ^ k) for i in range(count)])
        for k in range(count - 1, 0, -1)
    }
    return [blocks[0]] + [swapped[k] for k in range(1, count)]


def expert_kernel(*refs, peers, count):
    row_refs, sources, out_refs = refs[:peers], refs[peers : peers + count], refs[peers + count :]
    out_refs, held = out_refs[:peers], out_refs[peers:]
    rows_held, hidden_ref, down_ref, arrivals = held[-4:]
    units = sources[2].shape[0]
    down_places = [down_ref.at[pl.ds(units * part, units)] for part in range(count // 3)]
    held = [
        place
        for part, down_place in enumerate(down_places)
        for place in (held[2 * part], held[2 * part + 1], down_place)
    ]
    row_copies = [
        pltpu.make_async_copy(source, rows_held.at[peer], arrivals.at[count + peer])
        for peer, source in enumerate(row_refs)
    ]
    copies = [
        pltpu.make_async_copy(source, place, arrivals.at[number])
        for number, (source, place) in enumerate(zip(sources, held))
    ]
    ahead = [copies[part + half] for part in range(0, count, 3) for half in range(2)]
    ahead = ahead + [copies[part + 2] for part in range(0, count, 3)]
    for copy in row_copies + ahead[:2]:
        copy.start()
    for copy in row_copies:
        copy.wait()
    for copy in ahead[2:4]:
        copy.start()
    ahead = ahead[4:]
    chunk, width = row_refs[0].shape
    rows = rows_held[...].reshape(peers * chunk, width)
    for number in range(0, count, 3):
        copies[number].wait()
        gate_value = jnp.dot(rows, held[number][...], preferred_element_type=jnp.float32)
        copies[number + 1].wait()
        fresh, ahead = (ahead[:3], ahead[3:]) if number + 3 < count else (ahead, [])
        for copy in fresh:
            copy.start()
        up_value = jnp.dot(rows, held[number + 1][...], preferred_element_type=jnp.float32)
        hidden = (gate_value / (1.0 + jnp.exp(-gate_value)) * up_value).astype(jnp.bfloat16)
        first = number // 3 * units
        hidden_ref[:, first : first + units] = hidden
    for number in range(2, count, 3):
        copies[number].wait()
    total = jnp.dot(
        hidden_ref[...], down_ref[...], preferred_element_type=jnp.float32
    ).astype(jnp.bfloat16)
    for peer in range(peers):
        out_refs[peer][...] = total[peer * chunk : (peer + 1) * chunk]


def expert_chunk(blocks, parts):
    flat = [array for part in parts for array in part]
    peers = len(blocks)
    chunk, width = blocks[0].shape
    row_count = peers * chunk
    hidden_units = sum(part[0].shape[1] for part in parts)
    return pl.pallas_call(
        lambda *refs: expert_kernel(*refs, peers=peers, count=len(flat)),
        out_shape=[jax.ShapeDtypeStruct((chunk, width), jnp.bfloat16)] * peers,
        in_specs=[pl.BlockSpec(memory_space=pl.ANY)] * (peers + len(flat)),
        scratch_shapes=[
            pltpu.VMEM(array.shape, array.dtype) for part in parts for array in part[:2]
        ]
        + [
            pltpu.VMEM((peers, chunk, width), jnp.bfloat16),
            pltpu.VMEM((row_count, hidden_units), jnp.bfloat16),
            pltpu.VMEM((hidden_units, width), jnp.bfloat16),
            pltpu.SemaphoreType.DMA((len(flat) + peers,)),
        ],
        cost_estimate=pl.CostEstimate(
            flops=6 * row_count * width * hidden_units,
            bytes_accessed=sum(2 * array.size for array in flat) + 4 * row_count * width,
            transcendentals=row_count * hidden_units,
        ),
        name="expert",
    )(*blocks, *flat)


def combine_kernel(shares_ref, *refs, peers):
    block_refs, rest = refs[:peers], refs[peers:]
    out_ref = rest[-1]
    both = jnp.dot(
        shares_ref[...],
        jnp.concatenate([block[...] for block in block_refs], 0),
        preferred_element_type=jnp.float32,
    )
    row_count = out_ref.shape[0]
    total = both[:row_count] + both[row_count:]
    if len(rest) > 1:
        total = total + rest[0][...]
    out_ref[...] = total.astype(out_ref.dtype)


def combine(shares, blocks, earlier, kind):
    peers = len(blocks)
    chunk, width = blocks[0].shape
    row_count = shares.shape[0] // 2
    columns = width // 4
    return pl.pallas_call(
        lambda *refs: combine_kernel(*refs, peers=peers),
        out_shape=jax.ShapeDtypeStruct((row_count, width), kind),
        grid=(width // columns,),
        in_specs=[pl.BlockSpec(shares.shape, lambda i: (0, 0))]
        + [pl.BlockSpec((chunk, columns), lambda i: (0, i))] * peers
        + [pl.BlockSpec((row_count, columns), lambda i: (0, i))] * len(earlier),
        out_specs=pl.BlockSpec((row_count, columns), lambda i: (0, i)),
        cost_estimate=pl.CostEstimate(
            flops=4 * row_count * peers * chunk * width,
            bytes_accessed=2 * peers * chunk * width + 6 * row_count * width,
            transcendentals=0,
        ),
        name="combine",
    )(shares, *blocks, *earlier)


def attend_kernel(limits_ref, sinks_ref, query_ref, pairs_ref, out_ref, *, group_size):
    block = pl.program_id(0)
    step = WINDOW
    span = step + 2 * WINDOW
    wide = 2 * HEAD_DIM
    scale = HEAD_DIM ** (-0.5) * math.log2(math.e)
    query_at = lax.broadcasted_iota(jnp.int32, (step, span), 0)
    key_at = lax.broadcasted_iota(jnp.int32, (step, span), 1)
    band = (key_at >= query_at) & (key_at <= query_at + 2 * WINDOW)
    low_half = lax.broadcasted_iota(jnp.int32, (span, wide), 1) < HEAD_DIM
    for part in range(query_ref.shape[0] // step):
        first = pl.multiple_of(block * query_ref.shape[0] + part * step, step)
        allowed = (
            band & (key_at >= limits_ref[0] - first) & (key_at < limits_ref[1] - first)
        )
        for kv_head in range(pairs_ref.shape[1] // wide):
            pair = pairs_ref[pl.ds(first, span), kv_head * wide : (kv_head + 1) * wide]
            turned = jnp.concatenate([pair[:, HEAD_DIM:], pair[:, :HEAD_DIM]], axis=1)
            zero = jnp.zeros_like(pair)
            keys = (jnp.where(low_half, pair, zero), jnp.where(low_half, zero, turned))
            values = (jnp.where(low_half, turned, zero), jnp.where(low_half, zero, pair))
            for two in range(group_size // 2):
                column = (kv_head * group_size + 2 * two) * HEAD_DIM
                query = query_ref[part * step : (part + 1) * step, column : column + wide]
                both = None
                for side in range(2):
                    sink = sinks_ref[kv_head * group_size + 2 * two + side]
                    scores = lax.dot_general(
                        query,
                        keys[side],
                        (((1,), (1,)), ((), ())),
                        preferred_element_type=jnp.float32,
                    )
                    scores = jnp.where(allowed, scores * scale, NEG_FILL)
                    top = jnp.maximum(jnp.max(scores, -1, keepdims=True), sink)
                    grown = jnp.exp2(scores - top)
                    denominator = jnp.sum(grown, -1, keepdims=True) + jnp.exp2(sink - top)
                    head = jnp.dot(
                        grown.astype(jnp.bfloat16),
                        values[side],
                        preferred_element_type=jnp.float32,
                    ) * (1.0 / denominator)
                    both = head if both is None else both + head
                out_ref[part * step : (part + 1) * step, column : column + wide] = both.astype(
                    out_ref.dtype
                )


def attend(queries, padded, sink_logits):
    row_count, width = queries.shape
    kv_local = padded.shape[1] // (2 * HEAD_DIM)
    group_size = width // (kv_local * HEAD_DIM)
    block_rows = min(2 * WINDOW, row_count)
    offset = lax.axis_index("ep") * row_count
    seq_total = row_count * lax.axis_size("ep")
    limits = jnp.stack([WINDOW - offset, seq_total + WINDOW - offset]).astype(jnp.int32)
    heads = kv_local * group_size
    sinks = lax.dynamic_slice_in_dim(sink_logits, lax.axis_index("tp") * heads, heads, 0)
    return pl.pallas_call(
        lambda *refs: attend_kernel(*refs, group_size=group_size),
        out_shape=jax.ShapeDtypeStruct(queries.shape, jnp.bfloat16),
        grid=(row_count // block_rows,),
        in_specs=[
            pl.BlockSpec(memory_space=pltpu.SMEM),
            pl.BlockSpec(memory_space=pltpu.SMEM),
            pl.BlockSpec((block_rows, width), lambda i: (i, 0)),
            pl.BlockSpec(padded.shape, lambda i: (0, 0)),
        ],
        out_specs=pl.BlockSpec((block_rows, width), lambda i: (i, 0)),
        cost_estimate=pl.CostEstimate(
            flops=24 * row_count * width * WINDOW,
            bytes_accessed=4 * queries.size + 2 * padded.size,
            transcendentals=3 * row_count * heads * WINDOW,
        ),
        name="attend",
    )(limits, sinks * math.log2(math.e), queries, padded)


def layer(
    queries,
    keys_values,
    sink_logits,
    out_weight,
    expert_tokens,
    norm_gain,
    routes,
    route_weights,
    gate_weight,
    up_weight,
    down_weight,
):
    ep_count = lax.axis_size("ep")
    padded = padded_2(keys_values, (("ep", 0),), WINDOW)
    weights = gathered_parts((gate_weight[0], up_weight[0], down_weight[0]), "tp")

    row_count = expert_tokens.shape[0]
    capacity = 3 * row_count * TOPK // (2 * ep_count)
    chunk = -(-capacity // (CHUNKS * 16)) * 16

    order = lax.axis_index("ep") ^ jnp.arange(ep_count, dtype=jnp.int32)
    named_each = routes[:, :, None] == order
    named = jnp.any(named_each, 1)
    copy_weight = jnp.sum(jnp.where(named_each, route_weights[:, :, None], 0.0), 1)
    places = jnp.arange(row_count, dtype=jnp.int32)
    earlier = (places[None, :] < places[:, None]).astype(jnp.bfloat16)
    rank = jnp.dot(earlier, named.astype(jnp.bfloat16), preferred_element_type=jnp.float32)
    slot = jnp.where(named, rank.astype(jnp.int32), -1)

    sent = dispatch(expert_tokens, norm_gain, slot.T, chunk, CHUNKS)
    arrived = []
    for number in range(CHUNKS):
        arrived.append(exchange(sent[number], "ep"))

    attended = attend(queries, padded, sink_logits)
    tp_count = lax.axis_size("tp")
    mine = lax.axis_index("tp")
    own_rows = attended.shape[0] // tp_count
    width = attended.shape[1]
    mixer_sum = None
    for other in range(tp_count):
        rows = lax.dynamic_slice_in_dim(attended, (mine ^ other) * own_rows, own_rows, 0)
        if other:
            rows = lax.ppermute(rows, "tp", [(i, i ^ other) for i in range(tp_count)])
        part = jnp.dot(
            rows,
            lax.dynamic_slice_in_dim(out_weight, (mine ^ other) * width, width, 0),
            preferred_element_type=jnp.float32,
        )
        mixer_sum = part if mixer_sum is None else mixer_sum + part
    mixer_out = mixer_sum.astype(jnp.bfloat16)

    gathered = ()
    for number in range(CHUNKS):
        results = expert_chunk(arrived[number], weights)
        returned = exchange(results, "ep")
        slots = number * chunk + jnp.arange(chunk, dtype=jnp.int32)
        share = jnp.where(
            slot[:, :, None] == slots[None, None, :], copy_weight[:, :, None], 0.0
        ).reshape(row_count, ep_count * chunk)
        share_high = lax.reduce_precision(share, 8, 7)
        shares = jnp.concatenate([share_high, share - share_high], 0).astype(jnp.bfloat16)
        last = number == CHUNKS - 1
        gathered = (
            combine(shares, returned, gathered, jnp.bfloat16 if last else jnp.float32),
        )
    return (mixer_out, gathered[0])


def solution(mesh):
    return jax.shard_map(
        layer,
        mesh=mesh,
        in_specs=(
            P("ep", "tp"),
            P("ep", "tp"),
            P(),
            P(),
            P(("ep", "tp"), None),
            P(),
            P(("ep", "tp"), None),
            P(("ep", "tp"), None),
            P("ep", None, "tp"),
            P("ep", None, "tp"),
            P("ep", "tp", None),
        ),
        out_specs=(P(("ep", "tp"), None), P(("ep", "tp"), None)),
        check_vma=False,
    )
```
